32 devices in a mesh: row: 4 (over y, x), col: 8 (over z, core).
Axes of the slice: x: 2, y: 2, z: 4, core: 2. Of those that a mesh axis runs over, the one named last changes fastest.
Arguments:
- mix_input: bfloat16 [4, 4096, 512], P(None, ('row', 'col')), may hold values from -6 to 6
- group_maps: bfloat16 [4, 128, 128], replicated, may hold values from -0.5 to 0.5
- out_map: bfloat16 [512, 2048], replicated, may hold values from -0.25 to 0.25
Outputs:
- mixed: bfloat16 [4, 4096, 2048], P(None, ('row', 'col'))
The draws below stay inside these ranges and needn't reach their ends.
All inputs are finite; a program needn't handle non-finite values.
Results may differ from the reference program's by a relative error of at most 0.011.
Values may be sent and summed in bfloat16 or wider, within the bound.
A program may use at most 64 MiB of HBM per device.

```python
import jax
import jax.numpy as jnp
from jax import lax

MODEL = 2048
GROUPS = 4
GROUP_CH = 128
SEQS = 4
CHANNELS = 512
LENGTH = 4096


def level_of(stream_key, shape, cuts, low, high):
    gain, own = 1.0, jax.random.fold_in(stream_key, 6)
    for axis_at, parts in cuts:
        heights = jnp.exp(jax.random.uniform(jax.random.fold_in(own, axis_at), (parts,), jnp.float32, low / len(cuts), high / len(cuts)))
        gain = gain * jnp.repeat(heights, shape[axis_at] // parts).reshape([-1 if axis == axis_at else 1 for axis in range(len(shape))])
    return gain


def centred(stream_key, dims, width, reach, shards=(), held_as=jnp.bfloat16):
    values = jax.random.normal(stream_key, dims, jnp.float32) * width
    if len(shards) > 0:
        values = level_of(stream_key, dims, shards, -0.22, 0.18) * values
    return jnp.clip(values, min=-reach, max=reach).astype(held_as)


def setup_inputs(seed: int = 0) -> dict:
    key_of = jax.random.split(jax.random.key(seed), 4)
    return {
        "mix_input": centred(key_of[0], (SEQS, LENGTH, CHANNELS), 1.0, 6.0, ((1, 32),)),
        "group_maps": centred(key_of[1], (GROUPS, GROUP_CH, GROUP_CH), GROUP_CH ** -0.5, 0.5),
        "out_map": centred(key_of[2], (CHANNELS, MODEL), CHANNELS ** -0.5, 0.25),
    }


def reference(mix_input, group_maps, out_map):
    def one_sequence(sequence):
        signal = sequence.astype(jnp.float32).reshape(LENGTH, GROUPS, GROUP_CH)
        spectrum = jnp.fft.fft2(signal, axes=(0, 2), norm="ortho").real.astype(jnp.float32)
        spectrum = spectrum.astype(jnp.bfloat16)
        grouped = jnp.einsum("pgj,gjl->pgl", spectrum.astype(jnp.float32), group_maps.astype(jnp.float32))
        grouped = grouped.astype(jnp.bfloat16).reshape(LENGTH, CHANNELS)
        return jnp.dot(grouped, out_map, preferred_element_type=jnp.float32).astype(jnp.bfloat16)

    return lax.map(one_sequence, mix_input)
```

```python
import math

import jax
import jax.numpy as jnp
import numpy as np
from jax import lax
from jax.sharding import PartitionSpec as P

AXES = ("row", "col")


def turn_tables(left_count, right_count, modulus):
    turns = np.arange(left_count)[:, None] * np.arange(right_count)[None, :] % modulus
    angles = turns * (2.0 * math.pi / modulus)
    return np.cos(angles), np.sin(angles)


def lane_tables(width):
    cosine, sine = turn_tables(width, width, width)
    half = width // 2
    pack = np.zeros((width, width))
    unpack = np.zeros((width, width))
    pack[:, 0::2] = cosine[:, :half]
    pack[:, 1::2] = -sine[:, :half]
    pack[:, 1] = cosine[:, half]
    unpack[0, 0] = 1.0
    unpack[1, half] = 1.0
    for freq in range(1, half):
        unpack[2 * freq, freq] = unpack[2 * freq, width - freq] = 1.0
        unpack[2 * freq + 1, freq] = 1.0
        unpack[2 * freq + 1, width - freq] = -1.0
    return pack, unpack


def per_device(mix_input, group_maps, out_map):
    bf16, f32 = jnp.bfloat16, jnp.float32
    seqs, positions, channels = mix_input.shape
    groups, width, _ = group_maps.shape
    devices = lax.axis_size("row") * lax.axis_size("col")
    me = lax.axis_index("row") * lax.axis_size("col") + lax.axis_index("col")
    length = devices * positions
    items = seqs * channels // devices
    pack, unpack = lane_tables(width)

    lanes = jnp.einsum(
        "spgj,jc->sgcp",
        mix_input.reshape(seqs, positions, groups, width),
        jnp.asarray(pack, bf16),
        preferred_element_type=f32,
    ).astype(bf16)
    sent = lanes.reshape(devices, items, positions)
    held = lax.all_to_all(sent, AXES, split_axis=0, concat_axis=0, tiled=True)

    dev_cos, dev_sin = turn_tables(devices, devices, devices)
    both = jnp.asarray(np.concatenate([dev_cos, -dev_sin], axis=1), bf16)
    spun = jnp.einsum("df,dnp->fnp", both, held, preferred_element_type=f32)
    real_in, imag_in = spun[:devices], spun[devices:]
    twist_cos, twist_sin = turn_tables(devices, positions, length)
    twist_cos = jnp.asarray(twist_cos, f32)[:, None, :]
    twist_sin = jnp.asarray(twist_sin, f32)[:, None, :]
    real_part = real_in * twist_cos + imag_in * twist_sin
    imag_part = imag_in * twist_cos - real_in * twist_sin
    lane_ids = (me * items + jnp.arange(items, dtype=jnp.int32)) % width
    is_sine = ((lane_ids % 2 == 1) & (lane_ids != 1))[None, :, None]
    first = jnp.where(is_sine, -imag_part, real_part).astype(bf16)
    second = jnp.where(is_sine, real_part, imag_part).astype(bf16)
    stacked = jnp.concatenate([first, second], axis=2)
    pos_cos, pos_sin = turn_tables(positions, positions, positions)
    scale = 1.0 / math.sqrt(length * width)
    pos_table = jnp.asarray(np.concatenate([pos_cos, pos_sin], axis=0) * scale, bf16)
    freqs = jnp.einsum("pm,fnp->mfn", pos_table, stacked, preferred_element_type=f32).astype(bf16)

    freqs = freqs.reshape(devices, positions, items)
    back = lax.all_to_all(freqs, AXES, split_axis=0, concat_axis=0, tiled=True)
    parts = width // items
    back = back.reshape(seqs, groups, parts, positions, items)
    back = back.transpose(0, 3, 1, 2, 4).reshape(seqs * positions, groups, width)
    maps = jnp.einsum(
        "cl,glm->gcm", jnp.asarray(unpack, bf16), group_maps, preferred_element_type=f32
    ).astype(bf16)
    grouped = jnp.einsum("rgc,gcm->rgm", back, maps, preferred_element_type=f32).astype(bf16)
    mixed = jnp.dot(
        grouped.reshape(seqs * positions, channels), out_map, preferred_element_type=f32
    )
    return mixed.astype(bf16).reshape(seqs, positions, out_map.shape[1])


def solution(mesh):
    return jax.shard_map(
        per_device,
        mesh=mesh,
        in_specs=(P(None, AXES, None), P(), P()),
        out_specs=P(None, AXES, None),
        check_vma=False,
    )
```

```python
import math

import jax
import jax.numpy as jnp
import numpy as np
from jax import lax
from jax.experimental import pallas as pl
from jax.experimental.pallas import tpu as pltpu
from jax.sharding import PartitionSpec as P

AXES = ("row", "col")


def turn_tables(left_count, right_count, modulus):
    turns = np.arange(left_count)[:, None] * np.arange(right_count)[None, :] % modulus
    angles = turns * (2.0 * math.pi / modulus)
    return np.cos(angles), np.sin(angles)


def lane_tables(width):
    cosine, sine = turn_tables(width, width, width)
    half = width // 2
    pack = np.zeros((width, width))
    unpack = np.zeros((width, width))
    pack[:, 0::2] = cosine[:, :half]
    pack[:, 1::2] = -sine[:, :half]
    pack[:, 1] = cosine[:, half]
    unpack[0, 0] = 1.0
    unpack[1, half] = 1.0
    for freq in range(1, half):
        unpack[2 * freq, freq] = unpack[2 * freq, width - freq] = 1.0
        unpack[2 * freq + 1, freq] = 1.0
        unpack[2 * freq + 1, width - freq] = -1.0
    return pack, unpack


def fourier(values):
    count = len(values)
    if count == 1:
        return values
    even, odd = fourier(values[0::2]), fourier(values[1::2])
    low, high = [], []
    for at in range(count // 2):
        cosine = math.cos(2.0 * math.pi * at / count)
        sine = math.sin(2.0 * math.pi * at / count)
        (even_re, even_im), (odd_re, odd_im) = even[at], odd[at]
        if at == 0:
            turn_re, turn_im = odd_re, odd_im
        elif 4 * at == count:
            turn_re, turn_im = odd_im, -odd_re
        elif odd_im is None:
            turn_re, turn_im = odd_re * cosine, odd_re * -sine
        else:
            turn_re = odd_re * cosine + odd_im * sine
            turn_im = odd_im * cosine - odd_re * sine
        if turn_re is None:
            low_re = high_re = even_re
        else:
            low_re, high_re = even_re + turn_re, even_re - turn_re
        if turn_im is None:
            low_im = high_im = even_im
        elif even_im is None:
            low_im, high_im = turn_im, -turn_im
        else:
            low_im, high_im = even_im + turn_im, even_im - turn_im
        low.append((low_re, low_im))
        high.append((high_re, high_im))
    return low + high


def mixing_kernel(
    x_ref, pack_ref, cos_ref, sin_ref, table_ref, out_ref,
    send, held, stack, big, send_back, back, send_sem, recv_sem, send_back_sem, recv_back_sem,
):
    bf16, f32 = jnp.bfloat16, jnp.float32
    seqs, positions, channels = x_ref.shape
    devices, items, _ = send.shape
    width = pack_ref.shape[0]
    groups = channels // width
    cols = lax.axis_size("col")
    me = lax.axis_index("row") * cols + lax.axis_index("col")
    barrier = pltpu.get_barrier_semaphore()

    def peer_of(step):
        peer = lax.rem(me + step, devices)
        return peer, (lax.div(peer, cols), lax.rem(peer, cols))

    def greet(step, carry):
        pl.semaphore_signal(
            barrier, inc=1, device_id=peer_of(step)[1], device_id_type=pl.DeviceIdType.MESH
        )
        return carry

    lax.fori_loop(1, devices, greet, 0)
    rows_t = (((1,), (1,)), ((), ()))
    for s in range(seqs):
        for g in range(groups):
            lanes = lax.dot_general(
                pack_ref[...], x_ref[s, :, g * width : (g + 1) * width], rows_t,
                preferred_element_type=f32,
            ).astype(bf16)
            for half in range(2):
                send[(s * groups + g) * 2 + half] = lanes[half * items : (half + 1) * items]
    pl.semaphore_wait(barrier, devices - 1)

    def exchange(src, dst, out_sem, in_sem):
        def copy(step):
            peer, where = peer_of(step)
            return pltpu.make_async_remote_copy(
                src_ref=src.at[peer], dst_ref=dst.at[me], send_sem=out_sem.at[peer],
                recv_sem=in_sem.at[me], device_id=where, device_id_type=pl.DeviceIdType.MESH,
            )

        def arrival(step):
            peer, where = peer_of(step)
            return pltpu.make_async_remote_copy(
                src_ref=src.at[peer], dst_ref=dst.at[peer], send_sem=out_sem.at[peer],
                recv_sem=in_sem.at[peer], device_id=where, device_id_type=pl.DeviceIdType.MESH,
            )

        def start(step, carry):
            copy(step).start()
            return carry

        def finish(step, carry):
            arrival(step).wait_recv()
            copy(step).wait_send()
            return carry

        lax.fori_loop(1, devices, start, 0)
        dst[me] = src[me]
        lax.fori_loop(1, devices, finish, 0)

    exchange(send, held, send_sem, recv_sem)

    tile = 16
    def spin(chunk, carry):
        rows = pl.ds(pl.multiple_of(chunk * tile, tile), tile)
        spun = fourier([(held[d, rows, :].astype(f32), None) for d in range(devices)])
        row_ids = chunk * tile + lax.broadcasted_iota(jnp.int32, (tile, positions), 0)
        lane_ids = lax.rem(me * items + row_ids, width)
        is_sine = (lax.rem(lane_ids, 2) == 1) & (lane_ids != 1)
        for f in range(devices):
            real_in, imag_in = spun[f]
            cosine, sine = cos_ref[f : f + 1, :], sin_ref[f : f + 1, :]
            if imag_in is None:
                real_part, imag_part = real_in * cosine, -(real_in * sine)
            else:
                real_part = real_in * cosine + imag_in * sine
                imag_part = imag_in * cosine - real_in * sine
            stack[f, rows, :positions] = jnp.where(is_sine, -imag_part, real_part).astype(bf16)
            stack[f, rows, positions:] = jnp.where(is_sine, real_part, imag_part).astype(bf16)
        return carry

    lax.fori_loop(0, items // tile, spin, 0)
    pairs = devices // 2
    for a in range(pairs):
        both = jnp.concatenate([stack[a], stack[a + pairs]], axis=0)
        big[pl.ds(a, positions, stride=pairs), :] = lax.dot_general(
            table_ref[...], both, rows_t, preferred_element_type=f32
        )
    for e in range(devices):
        send_back[e] = big[e * items : (e + 1) * items, :].astype(bf16)

    exchange(send_back, back, send_back_sem, recv_back_sem)

    left = lax.broadcasted_iota(jnp.int32, (items, width), 1) < items
    for s in range(seqs):
        for g in range(groups):
            slot = (s * groups + g) * 2
            first, second = back[slot].astype(f32), back[slot + 1].astype(f32)
            halves = (
                jnp.where(left, first, pltpu.roll(second, items, 1)),
                jnp.where(left, pltpu.roll(first, items, 1), second),
            )
            for h in range(2):
                packed = halves[h].astype(bf16)
                for m in range(items // pairs):
                    base = m * devices + h * pairs
                    out_ref[s, base : base + pairs, g * width : (g + 1) * width] = packed[
                        m * pairs : (m + 1) * pairs
                    ]


def fused_lanes(mix_input, pack, devices, scale):
    bf16, f32 = jnp.bfloat16, jnp.float32
    seqs, positions, channels = mix_input.shape
    width = pack.shape[0]
    items = seqs * channels // devices
    length = devices * positions
    twist_cos, twist_sin = turn_tables(devices, positions, length)
    pos_cos, pos_sin = turn_tables(positions, positions, positions)
    table = np.concatenate([pos_cos, pos_sin], axis=1) * scale
    slots = (devices, items, positions)
    vmem = pl.BlockSpec(memory_space=pltpu.VMEM)
    dma = pltpu.SemaphoreType.DMA((devices,))
    return pl.pallas_call(
        mixing_kernel,
        out_shape=jax.ShapeDtypeStruct(mix_input.shape, bf16),
        in_specs=[vmem] * 5,
        out_specs=vmem,
        scratch_shapes=[
            pltpu.VMEM(slots, bf16), pltpu.VMEM(slots, bf16),
            pltpu.VMEM((devices, items, 2 * positions), bf16),
            pltpu.VMEM((devices * items, width), f32),
            pltpu.VMEM(slots, bf16), pltpu.VMEM(slots, bf16),
            dma, dma, dma, dma,
        ],
        compiler_params=pltpu.CompilerParams(
            collective_id=0, has_side_effects=True, vmem_limit_bytes=24 * 1024 * 1024
        ),
    )(
        mix_input, jnp.asarray(pack.T, bf16), jnp.asarray(twist_cos, f32),
        jnp.asarray(twist_sin, f32), jnp.asarray(table, bf16),
    )


def exchanged_lanes(mix_input, pack, width, devices, me, scale):
    bf16, f32 = jnp.bfloat16, jnp.float32
    seqs, positions, channels = mix_input.shape
    groups = channels // width
    length = devices * positions
    items = seqs * channels // devices
    lanes = jnp.einsum(
        "spgj,jc->sgcp",
        mix_input.reshape(seqs, positions, groups, width),
        jnp.asarray(pack, bf16),
        preferred_element_type=f32,
    ).astype(bf16)
    sent = lanes.reshape(devices, items, positions)
    held = lax.all_to_all(sent, AXES, split_axis=0, concat_axis=0, tiled=True)

    dev_cos, dev_sin = turn_tables(devices, devices, devices)
    both = jnp.asarray(np.concatenate([dev_cos, -dev_sin], axis=1), bf16)
    spun = jnp.einsum("df,dnp->fnp", both, held, preferred_element_type=f32)
    real_in, imag_in = spun[:devices], spun[devices:]
    twist_cos, twist_sin = turn_tables(devices, positions, length)
    twist_cos = jnp.asarray(twist_cos, f32)[:, None, :]
    twist_sin = jnp.asarray(twist_sin, f32)[:, None, :]
    real_part = real_in * twist_cos + imag_in * twist_sin
    imag_part = imag_in * twist_cos - real_in * twist_sin
    lane_ids = (me * items + jnp.arange(items, dtype=jnp.int32)) % width
    is_sine = ((lane_ids % 2 == 1) & (lane_ids != 1))[None, :, None]
    first = jnp.where(is_sine, -imag_part, real_part).astype(bf16)
    second = jnp.where(is_sine, real_part, imag_part).astype(bf16)
    stacked = jnp.concatenate([first, second], axis=2)
    pos_cos, pos_sin = turn_tables(positions, positions, positions)
    pos_table = jnp.asarray(np.concatenate([pos_cos, pos_sin], axis=0) * scale, bf16)
    freqs = jnp.einsum("pm,fnp->mfn", pos_table, stacked, preferred_element_type=f32).astype(bf16)

    freqs = freqs.reshape(devices, positions, items)
    back = lax.all_to_all(freqs, AXES, split_axis=0, concat_axis=0, tiled=True)
    parts = width // items
    back = back.reshape(seqs, groups, parts, positions, items)
    return back.transpose(0, 3, 1, 2, 4).reshape(seqs * positions, groups, width)


def per_device(mix_input, group_maps, out_map):
    bf16, f32 = jnp.bfloat16, jnp.float32
    seqs, positions, channels = mix_input.shape
    groups, width, _ = group_maps.shape
    devices = lax.axis_size("row") * lax.axis_size("col")
    me = lax.axis_index("row") * lax.axis_size("col") + lax.axis_index("col")
    items = seqs * channels // devices
    pack, unpack = lane_tables(width)
    scale = 1.0 / math.sqrt(devices * positions * width)
    if 2 * items == width and positions == width and items == 2 * devices:
        back = fused_lanes(mix_input, pack, devices, scale)
        back = back.reshape(seqs * positions, groups, width)
    else:
        back = exchanged_lanes(mix_input, pack, width, devices, me, scale)
    maps = jnp.einsum(
        "cl,glm->gcm", jnp.asarray(unpack, bf16), group_maps, preferred_element_type=f32
    ).astype(bf16)
    grouped = jnp.einsum("rgc,gcm->rgm", back, maps, preferred_element_type=f32).astype(bf16)
    mixed = jnp.dot(
        grouped.reshape(seqs * positions, channels), out_map, preferred_element_type=f32
    )
    return mixed.astype(bf16).reshape(seqs, positions, out_map.shape[1])


def solution(mesh):
    return jax.shard_map(
        per_device,
        mesh=mesh,
        in_specs=(P(None, AXES, None), P(), P()),
        out_specs=P(None, AXES, None),
        check_vma=False,
    )
```

```python
import math

import jax
import jax.numpy as jnp
import numpy as np
from jax import lax
from jax.experimental import pallas as pl
from jax.experimental.pallas import tpu as pltpu
from jax.sharding import PartitionSpec as P

AXES = ("row", "col")


def turn_tables(left_count, right_count, modulus):
    turns = np.arange(left_count)[:, None] * np.arange(right_count)[None, :] % modulus
    angles = turns * (2.0 * math.pi / modulus)
    return np.cos(angles), np.sin(angles)


def lane_tables(width):
    cosine, sine = turn_tables(width, width, width)
    half = width // 2
    pack = np.zeros((width, width))
    unpack = np.zeros((width, width))
    pack[:, 0::2] = cosine[:, :half]
    pack[:, 1::2] = -sine[:, :half]
    pack[:, 1] = cosine[:, half]
    unpack[0, 0] = 1.0
    unpack[1, half] = 1.0
    for freq in range(1, half):
        unpack[2 * freq, freq] = unpack[2 * freq, width - freq] = 1.0
        unpack[2 * freq + 1, freq] = 1.0
        unpack[2 * freq + 1, width - freq] = -1.0
    return pack, unpack


def fourier(values):
    count = len(values)
    if count == 1:
        return values
    even, odd = fourier(values[0::2]), fourier(values[1::2])
    low, high = [], []
    for at in range(count // 2):
        cosine = math.cos(2.0 * math.pi * at / count)
        sine = math.sin(2.0 * math.pi * at / count)
        (even_re, even_im), (odd_re, odd_im) = even[at], odd[at]
        if at == 0:
            turn_re, turn_im = odd_re, odd_im
        elif 4 * at == count:
            turn_re, turn_im = odd_im, -odd_re
        elif odd_im is None:
            turn_re, turn_im = odd_re * cosine, odd_re * -sine
        else:
            turn_re = odd_re * cosine + odd_im * sine
            turn_im = odd_im * cosine - odd_re * sine
        if turn_re is None:
            low_re = high_re = even_re
        else:
            low_re, high_re = even_re + turn_re, even_re - turn_re
        if turn_im is None:
            low_im = high_im = even_im
        elif even_im is None:
            low_im, high_im = turn_im, -turn_im
        else:
            low_im, high_im = even_im + turn_im, even_im - turn_im
        low.append((low_re, low_im))
        high.append((high_re, high_im))
    return low + high


def mixing_kernel(
    x_ref, pack_ref, cos_ref, sin_ref, table_ref, out_ref,
    send, held, stack, big, send_back, back, send_sem, recv_sem, send_back_sem, recv_back_sem,
):
    bf16, f32 = jnp.bfloat16, jnp.float32
    seqs, positions, channels = x_ref.shape
    devices, items, _ = send.shape
    width = pack_ref.shape[0]
    groups = channels // width
    cols = lax.axis_size("col")
    me = lax.axis_index("row") * cols + lax.axis_index("col")
    row, col = lax.axis_index("row"), lax.axis_index("col")
    row_count, span = devices // cols, cols // 2
    side = lax.div(col, span)
    half_count = devices // 2
    far, near = (0, half_count), (half_count + 1, devices)
    barrier = pltpu.get_barrier_semaphore()

    def peer_of(step):
        at = lax.rem(step, half_count)
        peer_side = lax.rem(side + 1 + lax.div(step, half_count), 2)
        peer_row = lax.rem(row + lax.div(at, span), row_count)
        peer_col = peer_side * span + lax.rem(col + at, span)
        return peer_row * cols + peer_col, (peer_row, peer_col)

    def each(steps, act):
        def body(step, carry):
            act(step)
            return carry

        lax.fori_loop(steps[0], steps[1], body, 0)

    def greet(step):
        pl.semaphore_signal(
            barrier, inc=1, device_id=peer_of(step)[1], device_id_type=pl.DeviceIdType.MESH
        )

    each(far, greet)
    each(near, greet)
    rows_t = (((1,), (1,)), ((), ()))
    for s in range(seqs):
        for g in range(groups):
            lanes = lax.dot_general(
                pack_ref[...], x_ref[s, :, g * width : (g + 1) * width], rows_t,
                preferred_element_type=f32,
            ).astype(bf16)
            for half in range(2):
                send[(s * groups + g) * 2 + half] = lanes[half * items : (half + 1) * items]
    pl.semaphore_wait(barrier, devices - 1)

    def move(src, dst, out_sem, in_sem, step, rows, part, arrives):
        peer, where = peer_of(step)
        slot = peer if arrives else me
        return pltpu.make_async_remote_copy(
            src_ref=src.at[peer, rows], dst_ref=dst.at[slot, rows],
            send_sem=out_sem.at[part, peer], recv_sem=in_sem.at[part, slot],
            device_id=where, device_id_type=pl.DeviceIdType.MESH,
        )

    chunks = send_sem.shape[0]
    chunk_rows = items // chunks
    whole = pl.ds(0, items)

    def outward(part, step, arrives):
        rows = pl.ds(part * chunk_rows, chunk_rows)
        return move(send, held, send_sem, recv_sem, step, rows, part, arrives)

    def homeward(step, arrives):
        return move(send_back, back, send_back_sem, recv_back_sem, step, whole, 0, arrives)

    for part in range(chunks):
        for steps in (far, near):
            each(steps, lambda step: outward(part, step, False).start())
    held[me] = send[me]

    tile = 16
    def spin(chunk, carry):
        rows = pl.ds(pl.multiple_of(chunk * tile, tile), tile)
        spun = fourier([(held[d, rows, :].astype(f32), None) for d in range(devices)])
        row_ids = chunk * tile + lax.broadcasted_iota(jnp.int32, (tile, positions), 0)
        lane_ids = lax.rem(me * items + row_ids, width)
        is_sine = (lax.rem(lane_ids, 2) == 1) & (lane_ids != 1)
        for f in range(devices):
            real_in, imag_in = spun[f]
            cosine, sine = cos_ref[f : f + 1, :], sin_ref[f : f + 1, :]
            if imag_in is None:
                real_part, imag_part = real_in * cosine, -(real_in * sine)
            else:
                real_part = real_in * cosine + imag_in * sine
                imag_part = imag_in * cosine - real_in * sine
            stack[f, rows, :positions] = jnp.where(is_sine, -imag_part, real_part).astype(bf16)
            stack[f, rows, positions:] = jnp.where(is_sine, real_part, imag_part).astype(bf16)
        return carry

    for part in range(chunks):
        for steps in (near, far):
            each(steps, lambda step: outward(part, step, True).wait_recv())
        tiles = chunk_rows // tile
        lax.fori_loop(part * tiles, (part + 1) * tiles, spin, 0)
    pairs = devices // 2
    group = span * positions // devices
    for other in (1, 0):
        half_side = lax.rem(side + other, 2)
        rows = [
            table_ref[pl.ds(pl.multiple_of((r * 2 + half_side) * group, group), group), :]
            for r in range(row_count)
        ]
        table = jnp.concatenate(rows, axis=0)
        for a in range(pairs):
            both = jnp.concatenate([stack[a], stack[a + pairs]], axis=0)
            big[other, pl.ds(a, positions // 2, stride=pairs), :] = lax.dot_general(
                table, both, rows_t, preferred_element_type=f32
            )
        for r in range(row_count):
            for c in range(span):
                at = (r * span + c) * items
                send_back[r * cols + half_side * span + c] = big[other, at : at + items, :].astype(bf16)
        each(far if other else near, lambda step: homeward(step, False).start())
    back[me] = send_back[me]
    for steps in (near, far):
        each(steps, lambda step: homeward(step, True).wait_recv())

    left = lax.broadcasted_iota(jnp.int32, (items, width), 1) < items
    for s in range(seqs):
        for g in range(groups):
            slot = (s * groups + g) * 2
            first, second = back[slot].astype(f32), back[slot + 1].astype(f32)
            halves = (
                jnp.where(left, first, pltpu.roll(second, items, 1)),
                jnp.where(left, pltpu.roll(first, items, 1), second),
            )
            for h in range(2):
                packed = halves[h].astype(bf16)
                for m in range(items // pairs):
                    base = m * devices + h * pairs
                    out_ref[s, base : base + pairs, g * width : (g + 1) * width] = packed[
                        m * pairs : (m + 1) * pairs
                    ]
    for steps in (far, near):
        for part in range(chunks):
            each(steps, lambda step: outward(part, step, False).wait_send())
        each(steps, lambda step: homeward(step, False).wait_send())


def fused_lanes(mix_input, pack, devices, scale):
    bf16, f32 = jnp.bfloat16, jnp.float32
    seqs, positions, channels = mix_input.shape
    width = pack.shape[0]
    items = seqs * channels // devices
    length = devices * positions
    twist_cos, twist_sin = turn_tables(devices, positions, length)
    pos_cos, pos_sin = turn_tables(positions, positions, positions)
    table = np.concatenate([pos_cos, pos_sin], axis=1) * scale
    slots = (devices, items, positions)
    vmem = pl.BlockSpec(memory_space=pltpu.VMEM)
    dma, dma_back = pltpu.SemaphoreType.DMA((2, devices)), pltpu.SemaphoreType.DMA((1, devices))
    return pl.pallas_call(
        mixing_kernel,
        out_shape=jax.ShapeDtypeStruct(mix_input.shape, bf16),
        in_specs=[vmem] * 5,
        out_specs=vmem,
        scratch_shapes=[
            pltpu.VMEM(slots, bf16), pltpu.VMEM(slots, bf16),
            pltpu.VMEM((devices, items, 2 * positions), bf16),
            pltpu.VMEM((2, devices * items // 2, width), f32),
            pltpu.VMEM(slots, bf16), pltpu.VMEM(slots, bf16),
            dma, dma, dma_back, dma_back,
        ],
        compiler_params=pltpu.CompilerParams(
            collective_id=0, has_side_effects=True, vmem_limit_bytes=24 * 1024 * 1024
        ),
    )(
        mix_input, jnp.asarray(pack.T, bf16), jnp.asarray(twist_cos, f32),
        jnp.asarray(twist_sin, f32), jnp.asarray(table, bf16),
    )


def exchanged_lanes(mix_input, pack, width, devices, me, scale):
    bf16, f32 = jnp.bfloat16, jnp.float32
    seqs, positions, channels = mix_input.shape
    groups = channels // width
    length = devices * positions
    items = seqs * channels // devices
    lanes = jnp.einsum(
        "spgj,jc->sgcp",
        mix_input.reshape(seqs, positions, groups, width),
        jnp.asarray(pack, bf16),
        preferred_element_type=f32,
    ).astype(bf16)
    sent = lanes.reshape(devices, items, positions)
    held = lax.all_to_all(sent, AXES, split_axis=0, concat_axis=0, tiled=True)

    dev_cos, dev_sin = turn_tables(devices, devices, devices)
    both = jnp.asarray(np.concatenate([dev_cos, -dev_sin], axis=1), bf16)
    spun = jnp.einsum("df,dnp->fnp", both, held, preferred_element_type=f32)
    real_in, imag_in = spun[:devices], spun[devices:]
    twist_cos, twist_sin = turn_tables(devices, positions, length)
    twist_cos = jnp.asarray(twist_cos, f32)[:, None, :]
    twist_sin = jnp.asarray(twist_sin, f32)[:, None, :]
    real_part = real_in * twist_cos + imag_in * twist_sin
    imag_part = imag_in * twist_cos - real_in * twist_sin
    lane_ids = (me * items + jnp.arange(items, dtype=jnp.int32)) % width
    is_sine = ((lane_ids % 2 == 1) & (lane_ids != 1))[None, :, None]
    first = jnp.where(is_sine, -imag_part, real_part).astype(bf16)
    second = jnp.where(is_sine, real_part, imag_part).astype(bf16)
    stacked = jnp.concatenate([first, second], axis=2)
    pos_cos, pos_sin = turn_tables(positions, positions, positions)
    pos_table = jnp.asarray(np.concatenate([pos_cos, pos_sin], axis=0) * scale, bf16)
    freqs = jnp.einsum("pm,fnp->mfn", pos_table, stacked, preferred_element_type=f32).astype(bf16)

    freqs = freqs.reshape(devices, positions, items)
    back = lax.all_to_all(freqs, AXES, split_axis=0, concat_axis=0, tiled=True)
    parts = width // items
    back = back.reshape(seqs, groups, parts, positions, items)
    return back.transpose(0, 3, 1, 2, 4).reshape(seqs * positions, groups, width)


def per_device(mix_input, group_maps, out_map):
    bf16, f32 = jnp.bfloat16, jnp.float32
    seqs, positions, channels = mix_input.shape
    groups, width, _ = group_maps.shape
    devices = lax.axis_size("row") * lax.axis_size("col")
    me = lax.axis_index("row") * lax.axis_size("col") + lax.axis_index("col")
    items = seqs * channels // devices
    pack, unpack = lane_tables(width)
    scale = 1.0 / math.sqrt(devices * positions * width)
    fits = 2 * items == width and positions == width and items == 2 * devices
    if fits and lax.axis_size("col") * positions == 32 * devices:
        back = fused_lanes(mix_input, pack, devices, scale)
        back = back.reshape(seqs * positions, groups, width)
    else:
        back = exchanged_lanes(mix_input, pack, width, devices, me, scale)
    maps = jnp.einsum(
        "cl,glm->gcm", jnp.asarray(unpack, bf16), group_maps, preferred_element_type=f32
    ).astype(bf16)
    grouped = jnp.einsum("rgc,gcm->rgm", back, maps, preferred_element_type=f32).astype(bf16)
    mixed = jnp.dot(
        grouped.reshape(seqs * positions, channels), out_map, preferred_element_type=f32
    )
    return mixed.astype(bf16).reshape(seqs, positions, out_map.shape[1])


def solution(mesh):
    return jax.shard_map(
        per_device,
        mesh=mesh,
        in_specs=(P(None, AXES, None), P(), P()),
        out_specs=P(None, AXES, None),
        check_vma=False,
    )
```

```python
import math

import jax
import jax.numpy as jnp
import numpy as np
from jax import lax
from jax.experimental import pallas as pl
from jax.experimental.pallas import tpu as pltpu
from jax.sharding import PartitionSpec as P

AXES = ("row", "col")


def turn_tables(left_count, right_count, modulus):
    turns = np.arange(left_count)[:, None] * np.arange(right_count)[None, :] % modulus
    angles = turns * (2.0 * math.pi / modulus)
    return np.cos(angles), np.sin(angles)


def lane_tables(width):
    cosine, sine = turn_tables(width, width, width)
    half = width // 2
    pack = np.zeros((width, width))
    unpack = np.zeros((width, width))
    pack[:, 0::2] = cosine[:, :half]
    pack[:, 1::2] = -sine[:, :half]
    pack[:, 1] = cosine[:, half]
    unpack[0, 0] = 1.0
    unpack[1, half] = 1.0
    for freq in range(1, half):
        unpack[2 * freq, freq] = unpack[2 * freq, width - freq] = 1.0
        unpack[2 * freq + 1, freq] = 1.0
        unpack[2 * freq + 1, width - freq] = -1.0
    return pack, unpack


def fourier(values):
    count = len(values)
    if count == 1:
        return values
    even, odd = fourier(values[0::2]), fourier(values[1::2])
    low, high = [], []
    for at in range(count // 2):
        cosine = math.cos(2.0 * math.pi * at / count)
        sine = math.sin(2.0 * math.pi * at / count)
        (even_re, even_im), (odd_re, odd_im) = even[at], odd[at]
        if at == 0:
            turn_re, turn_im = odd_re, odd_im
        elif 4 * at == count:
            turn_re, turn_im = odd_im, -odd_re
        elif odd_im is None:
            turn_re, turn_im = odd_re * cosine, odd_re * -sine
        else:
            turn_re = odd_re * cosine + odd_im * sine
            turn_im = odd_im * cosine - odd_re * sine
        if turn_re is None:
            low_re = high_re = even_re
        else:
            low_re, high_re = even_re + turn_re, even_re - turn_re
        if turn_im is None:
            low_im = high_im = even_im
        elif even_im is None:
            low_im, high_im = turn_im, -turn_im
        else:
            low_im, high_im = even_im + turn_im, even_im - turn_im
        low.append((low_re, low_im))
        high.append((high_re, high_im))
    return low + high


def mixing_kernel(
    x_hbm, pack_hbm, cos_hbm, sin_hbm, table_hbm, out_ref,
    x_ref, pack_ref, cos_ref, sin_ref, table_ref, load_sem,
    send, held, stack, big, send_back, back, send_sem, recv_sem, send_back_sem, recv_back_sem,
):
    bf16, f32 = jnp.bfloat16, jnp.float32
    seqs, positions, channels = x_ref.shape
    devices, items, _ = send.shape
    width = pack_ref.shape[0]
    groups = channels // width
    cols = lax.axis_size("col")
    me = lax.axis_index("row") * cols + lax.axis_index("col")
    far_refs = (x_hbm, pack_hbm, cos_hbm, sin_hbm, table_hbm)
    near_refs = (x_ref, pack_ref, cos_ref, sin_ref, table_ref)
    loads = [
        pltpu.make_async_copy(src, dst, load_sem.at[at])
        for at, (src, dst) in enumerate(zip(far_refs, near_refs))
    ]
    for load in loads:
        load.start()
    barrier = pltpu.get_barrier_semaphore()

    def peer_of(step):
        peer = lax.rem(me + step, devices)
        return peer, (lax.div(peer, cols), lax.rem(peer, cols))

    def greet(step, carry):
        pl.semaphore_signal(
            barrier, inc=1, device_id=peer_of(step)[1], device_id_type=pl.DeviceIdType.MESH
        )
        return carry

    lax.fori_loop(1, devices, greet, 0)
    rows_t = (((1,), (1,)), ((), ()))
    loads[0].wait()
    loads[1].wait()
    for s in range(seqs):
        for g in range(groups):
            lanes = lax.dot_general(
                pack_ref[...], x_ref[s, :, g * width : (g + 1) * width], rows_t,
                preferred_element_type=f32,
            ).astype(bf16)
            for half in range(2):
                send[(s * groups + g) * 2 + half] = lanes[half * items : (half + 1) * items]
    pl.semaphore_wait(barrier, devices - 1)

    def exchange(src, dst, out_sem, in_sem):
        def copy(step):
            peer, where = peer_of(step)
            return pltpu.make_async_remote_copy(
                src_ref=src.at[peer], dst_ref=dst.at[me], send_sem=out_sem.at[peer],
                recv_sem=in_sem.at[me], device_id=where, device_id_type=pl.DeviceIdType.MESH,
            )

        def arrival(step):
            peer, where = peer_of(step)
            return pltpu.make_async_remote_copy(
                src_ref=src.at[peer], dst_ref=dst.at[peer], send_sem=out_sem.at[peer],
                recv_sem=in_sem.at[peer], device_id=where, device_id_type=pl.DeviceIdType.MESH,
            )

        def start(step, carry):
            copy(step).start()
            return carry

        def finish(step, carry):
            arrival(step).wait_recv()
            copy(step).wait_send()
            return carry

        lax.fori_loop(1, devices, start, 0)
        dst[me] = src[me]
        lax.fori_loop(1, devices, finish, 0)

    exchange(send, held, send_sem, recv_sem)
    for load in loads[2:]:
        load.wait()

    tile = 16
    def spin(chunk, carry):
        rows = pl.ds(pl.multiple_of(chunk * tile, tile), tile)
        spun = fourier([(held[d, rows, :].astype(f32), None) for d in range(devices)])
        row_ids = chunk * tile + lax.broadcasted_iota(jnp.int32, (tile, positions), 0)
        lane_ids = lax.rem(me * items + row_ids, width)
        is_sine = (lax.rem(lane_ids, 2) == 1) & (lane_ids != 1)
        for f in range(devices):
            real_in, imag_in = spun[f]
            cosine, sine = cos_ref[f : f + 1, :], sin_ref[f : f + 1, :]
            if imag_in is None:
                real_part, imag_part = real_in * cosine, -(real_in * sine)
            else:
                real_part = real_in * cosine + imag_in * sine
                imag_part = imag_in * cosine - real_in * sine
            stack[f, rows, :positions] = jnp.where(is_sine, -imag_part, real_part).astype(bf16)
            stack[f, rows, positions:] = jnp.where(is_sine, real_part, imag_part).astype(bf16)
        return carry

    lax.fori_loop(0, items // tile, spin, 0)
    pairs = devices // 2
    for a in range(pairs):
        both = jnp.concatenate([stack[a], stack[a + pairs]], axis=0)
        big[pl.ds(a, positions, stride=pairs), :] = lax.dot_general(
            table_ref[...], both, rows_t, preferred_element_type=f32
        )
    for e in range(devices):
        send_back[e] = big[e * items : (e + 1) * items, :].astype(bf16)

    exchange(send_back, back, send_back_sem, recv_back_sem)

    left = lax.broadcasted_iota(jnp.int32, (items, width), 1) < items
    for s in range(seqs):
        for g in range(groups):
            slot = (s * groups + g) * 2
            first, second = back[slot].astype(f32), back[slot + 1].astype(f32)
            halves = (
                jnp.where(left, first, pltpu.roll(second, items, 1)),
                jnp.where(left, pltpu.roll(first, items, 1), second),
            )
            for h in range(2):
                packed = halves[h].astype(bf16)
                for m in range(items // pairs):
                    base = m * devices + h * pairs
                    out_ref[s, base : base + pairs, g * width : (g + 1) * width] = packed[
                        m * pairs : (m + 1) * pairs
                    ]


def fused_lanes(mix_input, pack, devices, scale):
    bf16, f32 = jnp.bfloat16, jnp.float32
    seqs, positions, channels = mix_input.shape
    width = pack.shape[0]
    items = seqs * channels // devices
    length = devices * positions
    twist_cos, twist_sin = turn_tables(devices, positions, length)
    pos_cos, pos_sin = turn_tables(positions, positions, positions)
    table = np.concatenate([pos_cos, pos_sin], axis=1) * scale
    slots = (devices, items, positions)
    vmem = pl.BlockSpec(memory_space=pltpu.VMEM)
    hbm = pl.BlockSpec(memory_space=pltpu.HBM)
    dma = pltpu.SemaphoreType.DMA((devices,))
    return pl.pallas_call(
        mixing_kernel,
        out_shape=jax.ShapeDtypeStruct(mix_input.shape, bf16),
        in_specs=[hbm] * 5,
        out_specs=vmem,
        scratch_shapes=[
            pltpu.VMEM(mix_input.shape, bf16), pltpu.VMEM(pack.shape, bf16),
            pltpu.VMEM(twist_cos.shape, f32), pltpu.VMEM(twist_sin.shape, f32),
            pltpu.VMEM(table.shape, bf16), pltpu.SemaphoreType.DMA((5,)),
            pltpu.VMEM(slots, bf16), pltpu.VMEM(slots, bf16),
            pltpu.VMEM((devices, items, 2 * positions), bf16),
            pltpu.VMEM((devices * items, width), f32),
            pltpu.VMEM(slots, bf16), pltpu.VMEM(slots, bf16),
            dma, dma, dma, dma,
        ],
        compiler_params=pltpu.CompilerParams(
            collective_id=0, has_side_effects=True
        ),
    )(
        mix_input, jnp.asarray(pack.T, bf16), jnp.asarray(twist_cos, f32),
        jnp.asarray(twist_sin, f32), jnp.asarray(table, bf16),
    )


def exchanged_lanes(mix_input, pack, width, devices, me, scale):
    bf16, f32 = jnp.bfloat16, jnp.float32
    seqs, positions, channels = mix_input.shape
    groups = channels // width
    length = devices * positions
    items = seqs * channels // devices
    lanes = jnp.einsum(
        "spgj,jc->sgcp",
        mix_input.reshape(seqs, positions, groups, width),
        jnp.asarray(pack, bf16),
        preferred_element_type=f32,
    ).astype(bf16)
    sent = lanes.reshape(devices, items, positions)
    held = lax.all_to_all(sent, AXES, split_axis=0, concat_axis=0, tiled=True)

    dev_cos, dev_sin = turn_tables(devices, devices, devices)
    both = jnp.asarray(np.concatenate([dev_cos, -dev_sin], axis=1), bf16)
    spun = jnp.einsum("df,dnp->fnp", both, held, preferred_element_type=f32)
    real_in, imag_in = spun[:devices], spun[devices:]
    twist_cos, twist_sin = turn_tables(devices, positions, length)
    twist_cos = jnp.asarray(twist_cos, f32)[:, None, :]
    twist_sin = jnp.asarray(twist_sin, f32)[:, None, :]
    real_part = real_in * twist_cos + imag_in * twist_sin
    imag_part = imag_in * twist_cos - real_in * twist_sin
    lane_ids = (me * items + jnp.arange(items, dtype=jnp.int32)) % width
    is_sine = ((lane_ids % 2 == 1) & (lane_ids != 1))[None, :, None]
    first = jnp.where(is_sine, -imag_part, real_part).astype(bf16)
    second = jnp.where(is_sine, real_part, imag_part).astype(bf16)
    stacked = jnp.concatenate([first, second], axis=2)
    pos_cos, pos_sin = turn_tables(positions, positions, positions)
    pos_table = jnp.asarray(np.concatenate([pos_cos, pos_sin], axis=0) * scale, bf16)
    freqs = jnp.einsum("pm,fnp->mfn", pos_table, stacked, preferred_element_type=f32).astype(bf16)

    freqs = freqs.reshape(devices, positions, items)
    back = lax.all_to_all(freqs, AXES, split_axis=0, concat_axis=0, tiled=True)
    parts = width // items
    back = back.reshape(seqs, groups, parts, positions, items)
    return back.transpose(0, 3, 1, 2, 4).reshape(seqs * positions, groups, width)


def per_device(mix_input, group_maps, out_map):
    bf16, f32 = jnp.bfloat16, jnp.float32
    seqs, positions, channels = mix_input.shape
    groups, width, _ = group_maps.shape
    devices = lax.axis_size("row") * lax.axis_size("col")
    me = lax.axis_index("row") * lax.axis_size("col") + lax.axis_index("col")
    items = seqs * channels // devices
    pack, unpack = lane_tables(width)
    scale = 1.0 / math.sqrt(devices * positions * width)
    if 2 * items == width and positions == width and items == 2 * devices:
        back = fused_lanes(mix_input, pack, devices, scale)
        back = back.reshape(seqs * positions, groups, width)
    else:
        back = exchanged_lanes(mix_input, pack, width, devices, me, scale)
    maps = jnp.einsum(
        "cl,glm->gcm", jnp.asarray(unpack, bf16), group_maps, preferred_element_type=f32
    ).astype(bf16)
    grouped = jnp.einsum("rgc,gcm->rgm", back, maps, preferred_element_type=f32).astype(bf16)
    mixed = jnp.dot(
        grouped.reshape(seqs * positions, channels), out_map, preferred_element_type=f32
    )
    return mixed.astype(bf16).reshape(seqs, positions, out_map.shape[1])


def solution(mesh):
    return jax.shard_map(
        per_device,
        mesh=mesh,
        in_specs=(P(None, AXES, None), P(), P()),
        out_specs=P(None, AXES, None),
        check_vma=False,
    )
```

```python
import math

import jax
import jax.numpy as jnp
import numpy as np
from jax import lax
from jax.experimental import pallas as pl
from jax.experimental.pallas import tpu as pltpu
from jax.sharding import PartitionSpec as P

AXES = ("row", "col")


def turn_tables(left_count, right_count, modulus):
    turns = np.arange(left_count)[:, None] * np.arange(right_count)[None, :] % modulus
    angles = turns * (2.0 * math.pi / modulus)
    return np.cos(angles), np.sin(angles)


def lane_tables(width):
    cosine, sine = turn_tables(width, width, width)
    half = width // 2
    pack = np.zeros((width, width))
    unpack = np.zeros((width, width))
    pack[:, 0::2] = cosine[:, :half]
    pack[:, 1::2] = -sine[:, :half]
    pack[:, 1] = cosine[:, half]
    unpack[0, 0] = 1.0
    unpack[1, half] = 1.0
    for freq in range(1, half):
        unpack[2 * freq, freq] = unpack[2 * freq, width - freq] = 1.0
        unpack[2 * freq + 1, freq] = 1.0
        unpack[2 * freq + 1, width - freq] = -1.0
    return pack, unpack


def fourier(values):
    count = len(values)
    if count == 1:
        return values
    even, odd = fourier(values[0::2]), fourier(values[1::2])
    low, high = [], []
    for at in range(count // 2):
        cosine = math.cos(2.0 * math.pi * at / count)
        sine = math.sin(2.0 * math.pi * at / count)
        (even_re, even_im), (odd_re, odd_im) = even[at], odd[at]
        if at == 0:
            turn_re, turn_im = odd_re, odd_im
        elif 4 * at == count:
            turn_re, turn_im = odd_im, -odd_re
        elif odd_im is None:
            turn_re, turn_im = odd_re * cosine, odd_re * -sine
        else:
            turn_re = odd_re * cosine + odd_im * sine
            turn_im = odd_im * cosine - odd_re * sine
        if turn_re is None:
            low_re = high_re = even_re
        else:
            low_re, high_re = even_re + turn_re, even_re - turn_re
        if turn_im is None:
            low_im = high_im = even_im
        elif even_im is None:
            low_im, high_im = turn_im, -turn_im
        else:
            low_im, high_im = even_im + turn_im, even_im - turn_im
        low.append((low_re, low_im))
        high.append((high_re, high_im))
    return low + high


def mixing_kernel(
    x_hbm, pack_hbm, cos_hbm, sin_hbm, table_hbm, unpack_hbm, given_hbm, out_ref,
    x_ref, pack_ref, cos_ref, sin_ref, table_ref, unpack_ref, given_ref, maps, load_sem,
    send, held, stack, big, send_back, back, send_sem, recv_sem, send_back_sem, recv_back_sem,
):
    bf16, f32 = jnp.bfloat16, jnp.float32
    seqs, positions, channels = x_ref.shape
    devices, items, _ = send.shape
    width = pack_ref.shape[0]
    groups = channels // width
    cols = lax.axis_size("col")
    me = lax.axis_index("row") * cols + lax.axis_index("col")
    far_refs = (x_hbm, pack_hbm, cos_hbm, sin_hbm, table_hbm, unpack_hbm, given_hbm)
    near_refs = (x_ref, pack_ref, cos_ref, sin_ref, table_ref, unpack_ref, given_ref)
    loads = [
        pltpu.make_async_copy(src, dst, load_sem.at[at])
        for at, (src, dst) in enumerate(zip(far_refs, near_refs))
    ]
    for load in loads:
        load.start()
    barrier = pltpu.get_barrier_semaphore()

    def peer_of(step):
        peer = lax.rem(me + step, devices)
        return peer, (lax.div(peer, cols), lax.rem(peer, cols))

    def greet(step, carry):
        pl.semaphore_signal(
            barrier, inc=1, device_id=peer_of(step)[1], device_id_type=pl.DeviceIdType.MESH
        )
        return carry

    lax.fori_loop(1, devices, greet, 0)
    rows_t = (((1,), (1,)), ((), ()))
    loads[0].wait()
    loads[1].wait()
    for s in range(seqs):
        for g in range(groups):
            lanes = lax.dot_general(
                pack_ref[...], x_ref[s, :, g * width : (g + 1) * width], rows_t,
                preferred_element_type=f32,
            ).astype(bf16)
            for half in range(2):
                send[(s * groups + g) * 2 + half] = lanes[half * items : (half + 1) * items]
    pl.semaphore_wait(barrier, devices - 1)

    def exchange(src, dst, out_sem, in_sem, beside):
        def copy(step):
            peer, where = peer_of(step)
            return pltpu.make_async_remote_copy(
                src_ref=src.at[peer], dst_ref=dst.at[me], send_sem=out_sem.at[peer],
                recv_sem=in_sem.at[me], device_id=where, device_id_type=pl.DeviceIdType.MESH,
            )

        def arrival(step):
            peer, where = peer_of(step)
            return pltpu.make_async_remote_copy(
                src_ref=src.at[peer], dst_ref=dst.at[peer], send_sem=out_sem.at[peer],
                recv_sem=in_sem.at[peer], device_id=where, device_id_type=pl.DeviceIdType.MESH,
            )

        def start(step, carry):
            copy(step).start()
            return carry

        def finish(step, carry):
            arrival(step).wait_recv()
            copy(step).wait_send()
            return carry

        lax.fori_loop(1, devices, start, 0)
        dst[me] = src[me]
        beside()
        lax.fori_loop(1, devices, finish, 0)

    def ready_maps():
        for load in loads[2:]:
            load.wait()
        for g in range(groups):
            maps[g] = jnp.dot(
                unpack_ref[...], given_ref[g], preferred_element_type=f32
            ).astype(bf16)

    exchange(send, held, send_sem, recv_sem, ready_maps)

    tile = 16
    def spin(chunk, carry):
        rows = pl.ds(pl.multiple_of(chunk * tile, tile), tile)
        spun = fourier([(held[d, rows, :].astype(f32), None) for d in range(devices)])
        row_ids = chunk * tile + lax.broadcasted_iota(jnp.int32, (tile, positions), 0)
        lane_ids = lax.rem(me * items + row_ids, width)
        is_sine = (lax.rem(lane_ids, 2) == 1) & (lane_ids != 1)
        for f in range(devices):
            real_in, imag_in = spun[f]
            cosine, sine = cos_ref[f : f + 1, :], sin_ref[f : f + 1, :]
            if imag_in is None:
                real_part, imag_part = real_in * cosine, -(real_in * sine)
            else:
                real_part = real_in * cosine + imag_in * sine
                imag_part = imag_in * cosine - real_in * sine
            stack[f, rows, :positions] = jnp.where(is_sine, -imag_part, real_part).astype(bf16)
            stack[f, rows, positions:] = jnp.where(is_sine, real_part, imag_part).astype(bf16)
        return carry

    lax.fori_loop(0, items // tile, spin, 0)
    pairs = devices // 2
    for a in range(pairs):
        both = jnp.concatenate([stack[a], stack[a + pairs]], axis=0)
        big[pl.ds(a, positions, stride=pairs), :] = lax.dot_general(
            table_ref[...], both, rows_t, preferred_element_type=f32
        )
    for e in range(devices):
        send_back[e] = big[e * items : (e + 1) * items, :].astype(bf16)

    exchange(send_back, back, send_back_sem, recv_back_sem, lambda: None)

    left = lax.broadcasted_iota(jnp.int32, (items, width), 1) < items
    for s in range(seqs):
        for g in range(groups):
            slot = (s * groups + g) * 2
            first, second = back[slot].astype(f32), back[slot + 1].astype(f32)
            halves = (
                jnp.where(left, first, pltpu.roll(second, items, 1)),
                jnp.where(left, pltpu.roll(first, items, 1), second),
            )
            for h in range(2):
                packed = jnp.dot(
                    halves[h].astype(bf16), maps[g], preferred_element_type=f32
                ).astype(bf16)
                for m in range(items // pairs):
                    base = m * devices + h * pairs
                    out_ref[s, base : base + pairs, g * width : (g + 1) * width] = packed[
                        m * pairs : (m + 1) * pairs
                    ]


def fused_lanes(mix_input, group_maps, pack, unpack, devices, scale):
    bf16, f32 = jnp.bfloat16, jnp.float32
    seqs, positions, channels = mix_input.shape
    width = pack.shape[0]
    items = seqs * channels // devices
    length = devices * positions
    twist_cos, twist_sin = turn_tables(devices, positions, length)
    pos_cos, pos_sin = turn_tables(positions, positions, positions)
    table = np.concatenate([pos_cos, pos_sin], axis=1) * scale
    slots = (devices, items, positions)
    vmem = pl.BlockSpec(memory_space=pltpu.VMEM)
    hbm = pl.BlockSpec(memory_space=pltpu.HBM)
    dma = pltpu.SemaphoreType.DMA((devices,))
    return pl.pallas_call(
        mixing_kernel,
        out_shape=jax.ShapeDtypeStruct(mix_input.shape, bf16),
        in_specs=[hbm] * 7,
        out_specs=vmem,
        scratch_shapes=[
            pltpu.VMEM(mix_input.shape, bf16), pltpu.VMEM(pack.shape, bf16),
            pltpu.VMEM(twist_cos.shape, f32), pltpu.VMEM(twist_sin.shape, f32),
            pltpu.VMEM(table.shape, bf16), pltpu.VMEM(unpack.shape, bf16),
            pltpu.VMEM(group_maps.shape, bf16), pltpu.VMEM(group_maps.shape, bf16),
            pltpu.SemaphoreType.DMA((7,)),
            pltpu.VMEM(slots, bf16), pltpu.VMEM(slots, bf16),
            pltpu.VMEM((devices, items, 2 * positions), bf16),
            pltpu.VMEM((devices * items, width), f32),
            pltpu.VMEM(slots, bf16), pltpu.VMEM(slots, bf16),
            dma, dma, dma, dma,
        ],
        compiler_params=pltpu.CompilerParams(
            collective_id=0, has_side_effects=True
        ),
    )(
        mix_input, jnp.asarray(pack.T, bf16), jnp.asarray(twist_cos, f32),
        jnp.asarray(twist_sin, f32), jnp.asarray(table, bf16), jnp.asarray(unpack, bf16), group_maps,
    )


def exchanged_lanes(mix_input, pack, width, devices, me, scale):
    bf16, f32 = jnp.bfloat16, jnp.float32
    seqs, positions, channels = mix_input.shape
    groups = channels // width
    length = devices * positions
    items = seqs * channels // devices
    lanes = jnp.einsum(
        "spgj,jc->sgcp",
        mix_input.reshape(seqs, positions, groups, width),
        jnp.asarray(pack, bf16),
        preferred_element_type=f32,
    ).astype(bf16)
    sent = lanes.reshape(devices, items, positions)
    held = lax.all_to_all(sent, AXES, split_axis=0, concat_axis=0, tiled=True)

    dev_cos, dev_sin = turn_tables(devices, devices, devices)
    both = jnp.asarray(np.concatenate([dev_cos, -dev_sin], axis=1), bf16)
    spun = jnp.einsum("df,dnp->fnp", both, held, preferred_element_type=f32)
    real_in, imag_in = spun[:devices], spun[devices:]
    twist_cos, twist_sin = turn_tables(devices, positions, length)
    twist_cos = jnp.asarray(twist_cos, f32)[:, None, :]
    twist_sin = jnp.asarray(twist_sin, f32)[:, None, :]
    real_part = real_in * twist_cos + imag_in * twist_sin
    imag_part = imag_in * twist_cos - real_in * twist_sin
    lane_ids = (me * items + jnp.arange(items, dtype=jnp.int32)) % width
    is_sine = ((lane_ids % 2 == 1) & (lane_ids != 1))[None, :, None]
    first = jnp.where(is_sine, -imag_part, real_part).astype(bf16)
    second = jnp.where(is_sine, real_part, imag_part).astype(bf16)
    stacked = jnp.concatenate([first, second], axis=2)
    pos_cos, pos_sin = turn_tables(positions, positions, positions)
    pos_table = jnp.asarray(np.concatenate([pos_cos, pos_sin], axis=0) * scale, bf16)
    freqs = jnp.einsum("pm,fnp->mfn", pos_table, stacked, preferred_element_type=f32).astype(bf16)

    freqs = freqs.reshape(devices, positions, items)
    back = lax.all_to_all(freqs, AXES, split_axis=0, concat_axis=0, tiled=True)
    parts = width // items
    back = back.reshape(seqs, groups, parts, positions, items)
    return back.transpose(0, 3, 1, 2, 4).reshape(seqs * positions, groups, width)


def per_device(mix_input, group_maps, out_map):
    bf16, f32 = jnp.bfloat16, jnp.float32
    seqs, positions, channels = mix_input.shape
    groups, width, _ = group_maps.shape
    devices = lax.axis_size("row") * lax.axis_size("col")
    me = lax.axis_index("row") * lax.axis_size("col") + lax.axis_index("col")
    items = seqs * channels // devices
    pack, unpack = lane_tables(width)
    scale = 1.0 / math.sqrt(devices * positions * width)
    if 2 * items == width and positions == width and items == 2 * devices:
        grouped = fused_lanes(mix_input, group_maps, pack, unpack, devices, scale)
    else:
        back = exchanged_lanes(mix_input, pack, width, devices, me, scale)
        maps = jnp.einsum(
            "cl,glm->gcm", jnp.asarray(unpack, bf16), group_maps, preferred_element_type=f32
        ).astype(bf16)
        grouped = jnp.einsum("rgc,gcm->rgm", back, maps, preferred_element_type=f32).astype(bf16)
    mixed = jnp.dot(
        grouped.reshape(seqs * positions, channels), out_map, preferred_element_type=f32
    )
    return mixed.astype(bf16).reshape(seqs, positions, out_map.shape[1])


def solution(mesh):
    return jax.shard_map(
        per_device,
        mesh=mesh,
        in_specs=(P(None, AXES, None), P(), P()),
        out_specs=P(None, AXES, None),
        check_vma=False,
    )
```

```python
import math

import jax
import jax.numpy as jnp
import numpy as np
from jax import lax
from jax.experimental import pallas as pl
from jax.experimental.pallas import tpu as pltpu
from jax.sharding import PartitionSpec as P

AXES = ("row", "col")


def turn_tables(left_count, right_count, modulus):
    turns = np.arange(left_count)[:, None] * np.arange(right_count)[None, :] % modulus
    angles = turns * (2.0 * math.pi / modulus)
    return np.cos(angles), np.sin(angles)


def lane_tables(width):
    cosine, sine = turn_tables(width, width, width)
    half = width // 2
    pack = np.zeros((width, width))
    unpack = np.zeros((width, width))
    pack[:, 0::2] = cosine[:, :half]
    pack[:, 1::2] = -sine[:, :half]
    pack[:, 1] = cosine[:, half]
    unpack[0, 0] = 1.0
    unpack[1, half] = 1.0
    for freq in range(1, half):
        unpack[2 * freq, freq] = unpack[2 * freq, width - freq] = 1.0
        unpack[2 * freq + 1, freq] = 1.0
        unpack[2 * freq + 1, width - freq] = -1.0
    return pack, unpack


def fourier(values):
    count = len(values)
    if count == 1:
        return values
    even, odd = fourier(values[0::2]), fourier(values[1::2])
    low, high = [], []
    for at in range(count // 2):
        cosine = math.cos(2.0 * math.pi * at / count)
        sine = math.sin(2.0 * math.pi * at / count)
        (even_re, even_im), (odd_re, odd_im) = even[at], odd[at]
        if at == 0:
            turn_re, turn_im = odd_re, odd_im
        elif 4 * at == count:
            turn_re, turn_im = odd_im, -odd_re
        elif odd_im is None:
            turn_re, turn_im = odd_re * cosine, odd_re * -sine
        else:
            turn_re = odd_re * cosine + odd_im * sine
            turn_im = odd_im * cosine - odd_re * sine
        if turn_re is None:
            low_re = high_re = even_re
        else:
            low_re, high_re = even_re + turn_re, even_re - turn_re
        if turn_im is None:
            low_im = high_im = even_im
        elif even_im is None:
            low_im, high_im = turn_im, -turn_im
        else:
            low_im, high_im = even_im + turn_im, even_im - turn_im
        low.append((low_re, low_im))
        high.append((high_re, high_im))
    return low + high


def mixing_kernel(
    x_hbm, pack_hbm, cos_hbm, sin_hbm, table_hbm, unpack_hbm, given_hbm, out_ref,
    x_ref, pack_ref, cos_ref, sin_ref, table_ref, unpack_ref, given_ref, maps, load_sem,
    send, held, stack, big, send_back, back, send_sem, recv_sem, send_back_sem, recv_back_sem,
):
    bf16, f32 = jnp.bfloat16, jnp.float32
    seqs, positions, channels = x_ref.shape
    devices, items, _ = send.shape
    width = pack_ref.shape[0]
    groups = channels // width
    cols = lax.axis_size("col")
    me = lax.axis_index("row") * cols + lax.axis_index("col")
    far_refs = (x_hbm, pack_hbm, cos_hbm, sin_hbm, table_hbm, unpack_hbm, given_hbm)
    near_refs = (x_ref, pack_ref, cos_ref, sin_ref, table_ref, unpack_ref, given_ref)
    loads = [
        pltpu.make_async_copy(src, dst, load_sem.at[at])
        for at, (src, dst) in enumerate(zip(far_refs, near_refs))
    ]
    for load in loads:
        load.start()
    barrier = pltpu.get_barrier_semaphore()

    def peer_of(step):
        peer = lax.rem(me + step, devices)
        return peer, (lax.div(peer, cols), lax.rem(peer, cols))

    def greet(step, carry):
        pl.semaphore_signal(
            barrier, inc=1, device_id=peer_of(step)[1], device_id_type=pl.DeviceIdType.MESH
        )
        return carry

    lax.fori_loop(1, devices, greet, 0)
    rows_t = (((1,), (1,)), ((), ()))
    loads[0].wait()
    loads[1].wait()
    for s in range(seqs):
        for g in range(groups):
            lanes = lax.dot_general(
                pack_ref[...], x_ref[s, :, g * width : (g + 1) * width], rows_t,
                preferred_element_type=f32,
            ).astype(bf16)
            for half in range(2):
                send[(s * groups + g) * 2 + half] = lanes[half * items : (half + 1) * items]
    pl.semaphore_wait(barrier, devices - 1)

    def exchange(src, dst, out_sem, in_sem, beside):
        def copy(step):
            peer, where = peer_of(step)
            return pltpu.make_async_remote_copy(
                src_ref=src.at[peer], dst_ref=dst.at[me], send_sem=out_sem.at[peer],
                recv_sem=in_sem.at[me], device_id=where, device_id_type=pl.DeviceIdType.MESH,
            )

        def arrival(step):
            peer, where = peer_of(step)
            return pltpu.make_async_remote_copy(
                src_ref=src.at[peer], dst_ref=dst.at[peer], send_sem=out_sem.at[peer],
                recv_sem=in_sem.at[peer], device_id=where, device_id_type=pl.DeviceIdType.MESH,
            )

        def start(step, carry):
            copy(step).start()
            return carry

        def finish(step, carry):
            arrival(step).wait_recv()
            copy(step).wait_send()
            return carry

        lax.fori_loop(1, devices, start, 0)
        dst[me] = src[me]
        beside()
        return copy, arrival, finish

    def ready_maps():
        for load in loads[2:]:
            load.wait()
        for g in range(groups):
            maps[g] = jnp.dot(
                unpack_ref[...], given_ref[g], preferred_element_type=f32
            ).astype(bf16)

    finish = exchange(send, held, send_sem, recv_sem, ready_maps)[2]
    lax.fori_loop(1, devices, finish, 0)

    tile = 16
    def spin(chunk, carry):
        rows = pl.ds(pl.multiple_of(chunk * tile, tile), tile)
        spun = fourier([(held[d, rows, :].astype(f32), None) for d in range(devices)])
        row_ids = chunk * tile + lax.broadcasted_iota(jnp.int32, (tile, positions), 0)
        lane_ids = lax.rem(me * items + row_ids, width)
        is_sine = (lax.rem(lane_ids, 2) == 1) & (lane_ids != 1)
        for f in range(devices):
            real_in, imag_in = spun[f]
            cosine, sine = cos_ref[f : f + 1, :], sin_ref[f : f + 1, :]
            if imag_in is None:
                real_part, imag_part = real_in * cosine, -(real_in * sine)
            else:
                real_part = real_in * cosine + imag_in * sine
                imag_part = imag_in * cosine - real_in * sine
            stack[f, rows, :positions] = jnp.where(is_sine, -imag_part, real_part).astype(bf16)
            stack[f, rows, positions:] = jnp.where(is_sine, real_part, imag_part).astype(bf16)
        return carry

    lax.fori_loop(0, items // tile, spin, 0)
    pairs = devices // 2
    for a in range(pairs):
        both = jnp.concatenate([stack[a], stack[a + pairs]], axis=0)
        big[pl.ds(a, positions, stride=pairs), :] = lax.dot_general(
            table_ref[...], both, rows_t, preferred_element_type=f32
        )
    for e in range(devices):
        send_back[e] = big[e * items : (e + 1) * items, :].astype(bf16)

    copy, arrival, _ = exchange(send_back, back, send_back_sem, recv_back_sem, lambda: None)

    left = lax.broadcasted_iota(jnp.int32, (items, width), 1) < items
    def settle(at, carry):
        pair = lax.rem(lax.div(me, 2) + pairs - at, pairs)
        slot = pair * 2
        for source in (slot, slot + 1):

            @pl.when(source != me)
            def _():
                arrival(lax.rem(source + devices - me, devices)).wait_recv()

        s, g = lax.div(pair, groups), lax.rem(pair, groups)
        lanes_at = pl.ds(pl.multiple_of(g * width, width), width)
        first, second = back[slot].astype(f32), back[slot + 1].astype(f32)
        halves = (
            jnp.where(left, first, pltpu.roll(second, items, 1)),
            jnp.where(left, pltpu.roll(first, items, 1), second),
        )
        for h in range(2):
            packed = jnp.dot(
                halves[h].astype(bf16), maps[g], preferred_element_type=f32
            ).astype(bf16)
            for m in range(items // pairs):
                base = m * devices + h * pairs
                out_ref[s, base : base + pairs, lanes_at] = packed[m * pairs : (m + 1) * pairs]
        return carry

    lax.fori_loop(0, pairs, settle, 0)

    def sent(step, carry):
        copy(step).wait_send()
        return carry

    lax.fori_loop(1, devices, sent, 0)


def fused_lanes(mix_input, group_maps, pack, unpack, devices, scale):
    bf16, f32 = jnp.bfloat16, jnp.float32
    seqs, positions, channels = mix_input.shape
    width = pack.shape[0]
    items = seqs * channels // devices
    length = devices * positions
    twist_cos, twist_sin = turn_tables(devices, positions, length)
    pos_cos, pos_sin = turn_tables(positions, positions, positions)
    table = np.concatenate([pos_cos, pos_sin], axis=1) * scale
    slots = (devices, items, positions)
    vmem = pl.BlockSpec(memory_space=pltpu.VMEM)
    hbm = pl.BlockSpec(memory_space=pltpu.HBM)
    dma = pltpu.SemaphoreType.DMA((devices,))
    return pl.pallas_call(
        mixing_kernel,
        out_shape=jax.ShapeDtypeStruct(mix_input.shape, bf16),
        in_specs=[hbm] * 7,
        out_specs=vmem,
        scratch_shapes=[
            pltpu.VMEM(mix_input.shape, bf16), pltpu.VMEM(pack.shape, bf16),
            pltpu.VMEM(twist_cos.shape, f32), pltpu.VMEM(twist_sin.shape, f32),
            pltpu.VMEM(table.shape, bf16), pltpu.VMEM(unpack.shape, bf16),
            pltpu.VMEM(group_maps.shape, bf16), pltpu.VMEM(group_maps.shape, bf16),
            pltpu.SemaphoreType.DMA((7,)),
            pltpu.VMEM(slots, bf16), pltpu.VMEM(slots, bf16),
            pltpu.VMEM((devices, items, 2 * positions), bf16),
            pltpu.VMEM((devices * items, width), f32),
            pltpu.VMEM(slots, bf16), pltpu.VMEM(slots, bf16),
            dma, dma, dma, dma,
        ],
        compiler_params=pltpu.CompilerParams(
            collective_id=0, has_side_effects=True
        ),
    )(
        mix_input, jnp.asarray(pack.T, bf16), jnp.asarray(twist_cos, f32),
        jnp.asarray(twist_sin, f32), jnp.asarray(table, bf16), jnp.asarray(unpack, bf16), group_maps,
    )


def exchanged_lanes(mix_input, pack, width, devices, me, scale):
    bf16, f32 = jnp.bfloat16, jnp.float32
    seqs, positions, channels = mix_input.shape
    groups = channels // width
    length = devices * positions
    items = seqs * channels // devices
    lanes = jnp.einsum(
        "spgj,jc->sgcp",
        mix_input.reshape(seqs, positions, groups, width),
        jnp.asarray(pack, bf16),
        preferred_element_type=f32,
    ).astype(bf16)
    sent = lanes.reshape(devices, items, positions)
    held = lax.all_to_all(sent, AXES, split_axis=0, concat_axis=0, tiled=True)

    dev_cos, dev_sin = turn_tables(devices, devices, devices)
    both = jnp.asarray(np.concatenate([dev_cos, -dev_sin], axis=1), bf16)
    spun = jnp.einsum("df,dnp->fnp", both, held, preferred_element_type=f32)
    real_in, imag_in = spun[:devices], spun[devices:]
    twist_cos, twist_sin = turn_tables(devices, positions, length)
    twist_cos = jnp.asarray(twist_cos, f32)[:, None, :]
    twist_sin = jnp.asarray(twist_sin, f32)[:, None, :]
    real_part = real_in * twist_cos + imag_in * twist_sin
    imag_part = imag_in * twist_cos - real_in * twist_sin
    lane_ids = (me * items + jnp.arange(items, dtype=jnp.int32)) % width
    is_sine = ((lane_ids % 2 == 1) & (lane_ids != 1))[None, :, None]
    first = jnp.where(is_sine, -imag_part, real_part).astype(bf16)
    second = jnp.where(is_sine, real_part, imag_part).astype(bf16)
    stacked = jnp.concatenate([first, second], axis=2)
    pos_cos, pos_sin = turn_tables(positions, positions, positions)
    pos_table = jnp.asarray(np.concatenate([pos_cos, pos_sin], axis=0) * scale, bf16)
    freqs = jnp.einsum("pm,fnp->mfn", pos_table, stacked, preferred_element_type=f32).astype(bf16)

    freqs = freqs.reshape(devices, positions, items)
    back = lax.all_to_all(freqs, AXES, split_axis=0, concat_axis=0, tiled=True)
    parts = width // items
    back = back.reshape(seqs, groups, parts, positions, items)
    return back.transpose(0, 3, 1, 2, 4).reshape(seqs * positions, groups, width)


def per_device(mix_input, group_maps, out_map):
    bf16, f32 = jnp.bfloat16, jnp.float32
    seqs, positions, channels = mix_input.shape
    groups, width, _ = group_maps.shape
    devices = lax.axis_size("row") * lax.axis_size("col")
    me = lax.axis_index("row") * lax.axis_size("col") + lax.axis_index("col")
    items = seqs * channels // devices
    pack, unpack = lane_tables(width)
    scale = 1.0 / math.sqrt(devices * positions * width)
    if 2 * items == width and positions == width and items == 2 * devices:
        grouped = fused_lanes(mix_input, group_maps, pack, unpack, devices, scale)
    else:
        back = exchanged_lanes(mix_input, pack, width, devices, me, scale)
        maps = jnp.einsum(
            "cl,glm->gcm", jnp.asarray(unpack, bf16), group_maps, preferred_element_type=f32
        ).astype(bf16)
        grouped = jnp.einsum("rgc,gcm->rgm", back, maps, preferred_element_type=f32).astype(bf16)
    mixed = jnp.dot(
        grouped.reshape(seqs * positions, channels), out_map, preferred_element_type=f32
    )
    return mixed.astype(bf16).reshape(seqs, positions, out_map.shape[1])


def solution(mesh):
    return jax.shard_map(
        per_device,
        mesh=mesh,
        in_specs=(P(None, AXES, None), P(), P()),
        out_specs=P(None, AXES, None),
        check_vma=False,
    )
```
